32 devices in a mesh: sp: 4 (over z), tp: 8 (over y, x, core).
Axes of the slice: x: 2, y: 2, z: 4, core: 2. Of those that a mesh axis runs over, the one named last changes fastest.
Arguments:
- stream: bfloat16 [1024, 4096], P('sp', 'tp'), may hold values from -80 to 80
- norm_gain: bfloat16 [3, 4096], replicated, may hold values from 0.099609375 to 1.8984375
- value_weight: bfloat16 [3, 2048, 4096], P(None, 'tp'), may hold values from -0.09375 to 0.09375
- gate_weight: bfloat16 [3, 2048, 4096], P(None, 'tp'), may hold values from -0.09375 to 0.09375
- kernel: float32 [3, 31, 2048], P(None, None, 'tp'), may hold values from -8 to 8
- kernel_bias: float32 [3, 2048], P(None, 'tp'), may hold values from -3 to 3
- chan_gain: float32 [3, 2048], P(None, 'tp'), may hold values from 0.1 to 1.9
- chan_shift: float32 [3, 2048], P(None, 'tp'), may hold values from -3 to 3
- out_weight: bfloat16 [3, 2048, 4096], P(None, None, 'tp'), may hold values from -0.125 to 0.125
Outputs:
- result: bfloat16 [1024, 4096], P('sp', 'tp')
The draws below stay inside these ranges and needn't reach their ends.
All inputs are finite; a program needn't handle non-finite values.
Results may differ from the reference program's by a relative error of at most 0.012.
Values may be sent and summed in bfloat16 or wider, within the bound.
No kernel may reach another device: no remote copies, remote signals or barrier semaphores. Data moves between devices by JAX's collectives and lax.ppermute only.
A program may use at most 64 MiB of HBM per device.

```python
import jax
import jax.numpy as jnp
from jax import lax

D = 4096
DC = 2048
KW = 31
LAYERS = 3
TOKENS = 1024


def draw_stream(key, part):
    keys = jax.random.split(jax.random.fold_in(key, 11), 3)
    noise = jnp.clip(jax.random.normal(keys[0], (TOKENS, D), jnp.float32), -4.0, 4.0)
    column_scale = jnp.exp(jnp.log(3.0) * jnp.arange(D, dtype=jnp.float32) / D + jax.random.uniform(keys[1], (D,), jnp.float32, -0.8, 0.8))
    row_scale = jnp.exp(jax.random.uniform(keys[2], (TOKENS, 1), jnp.float32, jnp.log(0.3), jnp.log(3.0)))
    return (noise * column_scale[None, :] * row_scale).astype(jnp.bfloat16)


def draw_kernel(key, part):
    keys = jax.random.split(jax.random.fold_in(key, 23), 2)
    noise = jnp.clip(jax.random.normal(keys[0], (LAYERS, KW, DC), jnp.float32), -4.0, 4.0)
    channel_scale = jnp.exp(jnp.log(6.0) * jnp.arange(DC, dtype=jnp.float32) / DC + jax.random.uniform(keys[1], (LAYERS, 1, DC), jnp.float32, -0.5, 0.5))
    return noise * channel_scale / jnp.sqrt(1.0 * KW)


def levels(stream_key, extent, cuts, low, largest):
    loudness, own = 1.0, jax.random.fold_in(stream_key, 6)
    for position, shards_of in cuts:
        steps = jnp.exp(jax.random.uniform(jax.random.fold_in(own, position), (shards_of,), jnp.float32, low / len(cuts), largest / len(cuts)))
        loudness = loudness * jnp.repeat(steps, extent[position] // shards_of).reshape([-1 if axis == position else 1 for axis in range(len(extent))])
    return loudness


def normal_values(stream_key, extent, width, most, shards=(), held_as=jnp.bfloat16):
    loudness = levels(stream_key, extent, shards, -0.22, 0.18) if shards else 1.0
    drawn = jax.random.normal(stream_key, extent, jnp.float32) * width * loudness
    return jnp.minimum(jnp.maximum(drawn, -most), most).astype(held_as)


def setup_inputs(seed: int = 0) -> dict:
    key_of = jax.random.split(jax.random.key(seed), 10)
    stream = draw_stream(jax.random.fold_in(key_of[9], 71), 0)
    norm_gain = jnp.clip(1.0 + 0.18 * jax.random.normal(key_of[1], (LAYERS, D), jnp.float32), 0.099609375, 1.8984375).astype(jnp.bfloat16)
    value_weight = normal_values(key_of[2], (LAYERS, DC, D), D ** -0.5, 0.09375, ((1, 8),))
    gate_weight = normal_values(key_of[3], (LAYERS, DC, D), D ** -0.5, 0.09375, ((1, 8),))
    kernel = draw_kernel(jax.random.fold_in(key_of[9], 71), 0)
    kernel_bias = normal_values(key_of[5], (LAYERS, DC), 0.5, 3.0, ((1, 8),), jnp.float32)
    chan_gain = jnp.clip(1.0 + 0.18 * jax.random.normal(key_of[6], (LAYERS, DC), jnp.float32), 0.1, 1.9)
    chan_shift = normal_values(key_of[7], (LAYERS, DC), 0.5, 3.0, ((1, 8),), jnp.float32)
    out_weight = normal_values(key_of[8], (LAYERS, DC, D), DC ** -0.5, 0.125, ((2, 8),))
    return {"stream": stream, "norm_gain": norm_gain, "value_weight": value_weight, "gate_weight": gate_weight, "kernel": kernel, "kernel_bias": kernel_bias, "chan_gain": chan_gain, "chan_shift": chan_shift, "out_weight": out_weight}


EPSILON = 1e-06

def against(left, right):
    return lax.dot_general(left, right, (((1,), (1,)), ((), ())), preferred_element_type=jnp.float32)

def reference(stream, norm_gain, value_weight, gate_weight, kernel, kernel_bias, chan_gain, chan_shift, out_weight):
    current = stream
    for layer_at in range(LAYERS):
        wide_rows = current.astype(jnp.float32)
        scale_row = lax.rsqrt(lax.optimization_barrier(jnp.mean(wide_rows * wide_rows, axis=1, keepdims=True)) + EPSILON)
        normed = (wide_rows * scale_row * norm_gain[layer_at].astype(jnp.float32)[None, :]).astype(jnp.bfloat16)
        value_part = against(normed, value_weight[layer_at])
        gate_part = against(normed, gate_weight[layer_at])
        gated_rows = (value_part * jax.nn.sigmoid(gate_part)).astype(jnp.bfloat16)
        padded = jnp.pad(gated_rows.astype(jnp.float32), ((KW - 1, 0), (0, 0)))
        convolved = jnp.broadcast_to(kernel_bias[layer_at][None, :], (TOKENS, DC))
        for tap_at in range(KW):
            convolved = convolved + kernel[layer_at, tap_at][None, :] * padded[tap_at:tap_at + TOKENS]
        centre = lax.optimization_barrier(jnp.mean(convolved, axis=1, keepdims=True))
        spread = lax.optimization_barrier(jnp.mean(convolved * convolved, axis=1, keepdims=True)) - centre * centre
        normal_out = (convolved - centre) * lax.rsqrt(spread + EPSILON) * chan_gain[layer_at][None, :] + chan_shift[layer_at][None, :]
        hidden = jax.nn.silu(normal_out).astype(jnp.bfloat16)
        projected = jnp.dot(hidden, out_weight[layer_at], preferred_element_type=jnp.float32)
        current = (current.astype(jnp.float32) + projected).astype(jnp.bfloat16)
    return current
```

```python
import functools

import jax
import jax.numpy as jnp
from jax import lax
from jax.experimental import pallas as pl
from jax.experimental.pallas import tpu as pltpu
from jax.sharding import PartitionSpec as P

EPSILON = 1e-06
TAIL = 16
LANES = 128
DIRECT_PEERS = 8
CHUNKS = 1
F32 = jnp.float32
BF16 = jnp.bfloat16


def up_to(count, unit):
    return -(-count // unit) * unit


def swapped(shard, by):
    count = lax.axis_size("tp")
    return lax.ppermute(shard, "tp", [(i, i ^ by) for i in range(count)])


def direct(count):
    return count <= DIRECT_PEERS and count & (count - 1) == 0


def source_order(count):
    if direct(count):
        return lax.axis_index("tp") ^ jnp.arange(count, dtype=jnp.int32)
    return jnp.arange(count, dtype=jnp.int32)


def fetched(shard):
    count = lax.axis_size("tp")
    if not direct(count):
        whole = lax.all_gather(shard, "tp", axis=0)
        return [whole[k] for k in range(count)]
    out = [None] * count
    for k in range(0, count, 2):
        out[k] = swapped(shard, k) if k else shard
    for k in range(0, count, 2):
        if k + 1 < count:
            out[k + 1] = swapped(out[k], 1)
    return out


def passed_along(shard):
    count = lax.axis_size("sp")
    return lax.ppermute(shard, "sp", [(i, i + 1) for i in range(count - 1)])


def vmem(count):
    return [pl.BlockSpec(memory_space=pltpu.VMEM)] * count


def smem():
    return pl.BlockSpec(memory_space=pltpu.SMEM)


def against(left, right):
    return lax.dot_general(
        left, right, (((1,), (1,)), ((), ())), preferred_element_type=F32
    )


def project_body(order_ref, gain_ref, value_ref, gate_ref, *refs, layer, count):
    shards, out_ref, last_ref = refs[:count], refs[count], refs[count + 1]
    width = shards[0].shape[1]
    squares = value = gate = None
    for k in range(count):
        at = pl.multiple_of(order_ref[k] * width, LANES)
        rows = shards[k][...]
        wide = rows.astype(F32)
        part = wide * wide
        folded = part[:, :LANES]
        for c in range(LANES, width, LANES):
            folded = folded + part[:, c : c + LANES]
        squares = folded if squares is None else squares + folded
        gains = gain_ref[layer : layer + 1, pl.ds(at, width)].astype(F32)
        ready = (wide * gains).astype(BF16)
        v = against(ready, value_ref[:, pl.ds(at, width)])
        g = against(ready, gate_ref[:, pl.ds(at, width)])
        value = v if value is None else value + v
        gate = g if gate is None else gate + g
    mean = jnp.sum(squares, axis=1, keepdims=True) / (width * count)
    scale = lax.rsqrt(mean + EPSILON)
    half = 0.5 * scale
    gated = ((value * half) * (1.0 + jnp.tanh(gate * half))).astype(BF16)
    out_ref[...] = gated
    last_ref[...] = gated[gated.shape[0] - last_ref.shape[0] :]


def project(order, norm_gain, value_matrix, gate_matrix, shards, layer, keep):
    rows, width = shards[0].shape
    channels = value_matrix.shape[0]
    count = len(shards)
    return pl.pallas_call(
        functools.partial(project_body, layer=layer, count=count),
        out_shape=(
            jax.ShapeDtypeStruct((rows, channels), BF16),
            jax.ShapeDtypeStruct((keep, channels), BF16),
        ),
        in_specs=[smem()] + vmem(3 + count),
        out_specs=tuple(vmem(2)),
        cost_estimate=pl.CostEstimate(
            flops=4 * rows * width * count * channels,
            bytes_accessed=2 * (rows + 2 * channels) * width * count,
            transcendentals=rows * channels,
        ),
        name="project",
    )(order, norm_gain, value_matrix, gate_matrix, *shards)


def convolve_body(kernel_ref, bias_ref, gain_ref, shift_ref, *refs, layer, spans, reach, rows, keep):
    parts, out_ref, line_ref = refs[: len(spans)], refs[len(spans)], refs[len(spans) + 1]
    channels = out_ref.shape[1]
    at = 0
    for ref, (low, high) in zip(parts, spans):
        line_ref[at : at + high - low, :] = ref[low:high, :].astype(F32)
        at += high - low
    step = 32
    taps = kernel_ref[layer]
    bias = bias_ref[layer : layer + 1, :]
    shifts = []
    for low in range(0, rows, step):
        total = jnp.broadcast_to(bias, (step, channels))
        for tap in range(reach + 1):
            start = low + keep - reach + tap
            total = total + taps[tap : tap + 1, :] * line_ref[start : start + step, :]
        local = jnp.mean(total, axis=1, keepdims=True).astype(BF16)
        out_ref[low : low + step, :] = (total - local.astype(F32)).astype(BF16)
        shifts.append(jnp.broadcast_to(local, (step, LANES)))
    shift = jnp.concatenate(shifts, axis=0)
    lane = lax.broadcasted_iota(jnp.int32, (rows, LANES), 1)
    shift = jnp.where(lane == 0, shift.astype(F32), 0.0).astype(BF16)
    row = lax.broadcasted_iota(jnp.int32, (TAIL, LANES), 0)
    tail_row = lax.broadcasted_iota(jnp.int32, (TAIL, channels), 0)
    used = min(rows, channels)
    tail = jnp.zeros((TAIL, used), F32)
    count = -(-rows // used)
    for j in range(count):
        tail = tail + against(
            (row == j).astype(F32).astype(BF16), shift[j * used : (j + 1) * used]
        )
    extra = jnp.zeros((TAIL, channels), F32)
    at = count
    for ref in (gain_ref, shift_ref):
        rest = 0.5 * ref[layer : layer + 1, :]
        for _ in range(3):
            piece = rest.astype(BF16).astype(F32)
            extra = jnp.where(tail_row == at, jnp.broadcast_to(piece, extra.shape), extra)
            rest = rest - piece
            at += 1
    if used < channels:
        tail = jnp.concatenate([tail, jnp.zeros((TAIL, channels - used), F32)], axis=1)
    out_ref[rows : rows + TAIL, :] = (tail + extra).astype(BF16)


def convolve(kernel, kernel_bias, chan_gain, chan_shift, parts, layer, keep):
    channels = kernel.shape[2]
    reach = kernel.shape[1] - 1
    total = sum(high - low for _, low, high in parts)
    rows = total - keep
    spans = [(low, high) for _, low, high in parts]
    return pl.pallas_call(
        functools.partial(
            convolve_body, layer=layer, spans=spans, reach=reach, rows=rows, keep=keep
        ),
        out_shape=jax.ShapeDtypeStruct((rows + TAIL, channels), BF16),
        in_specs=vmem(4 + len(parts)),
        out_specs=vmem(1)[0],
        scratch_shapes=[pltpu.VMEM((total, channels), F32)],
        cost_estimate=pl.CostEstimate(
            flops=2 * rows * channels * (reach + 1),
            bytes_accessed=4 * rows * channels,
            transcendentals=0,
        ),
        name="convolve",
    )(kernel, kernel_bias, chan_gain, chan_shift, *[p for p, _, _ in parts])


def emit_body(order_ref, weight_ref, *refs, spans, count, rows):
    shards = refs[:count]
    olds, out_ref = refs[count : count + len(spans)], refs[count + len(spans)]
    channels = shards[0].shape[1]
    used = min(rows, channels)
    pieces = -(-rows // used)
    row = lax.broadcasted_iota(jnp.int32, (TAIL, LANES), 0)
    picks = [(row == j).astype(F32).astype(BF16) for j in range(pieces)]
    ones = jnp.ones((channels, LANES), BF16)
    shifts, sums, squares = [], [], None
    for k in range(count):
        tail = shards[k][rows : rows + TAIL, :used]
        columns = [
            lax.dot_general(
                tail, pick, (((0,), (0,)), ((), ())), preferred_element_type=F32
            )
            for pick in picks
        ]
        shifts.append(jnp.concatenate(columns, axis=0) if pieces > 1 else columns[0])
        block = shards[k][:rows, :]
        sums.append(jnp.dot(block, ones, preferred_element_type=F32) / channels)
        wide = block.astype(F32)
        wide = wide * wide
        width = min(channels, LANES)
        folded = wide[:, :width]
        for c in range(width, channels, width):
            folded = folded + wide[:, c : c + width]
        squares = folded if squares is None else squares + folded
    centre = functools.reduce(jnp.add, [a + b for a, b in zip(shifts, sums)]) / count
    away = [a - centre for a in shifts]
    cross = functools.reduce(
        jnp.add, [d * (2.0 * s + d) for d, s in zip(away, sums)]
    ) / count
    spread = jnp.sum(squares, axis=1, keepdims=True) / (channels * count) + cross
    rate = lax.rsqrt(spread + EPSILON)
    total = None
    for k in range(count):
        extra = shards[k][rows : rows + TAIL, :].astype(F32)
        gain = extra[pieces : pieces + 1] + extra[pieces + 1 : pieces + 2] + extra[pieces + 2 : pieces + 3]
        shift = extra[pieces + 3 : pieces + 4] + extra[pieces + 4 : pieces + 5] + extra[pieces + 5 : pieces + 6]
        width = min(channels, LANES)
        offset = away[k][:, :width] * rate[:, :width]
        blocks = []
        for c in range(0, channels, width):
            values = shards[k][:rows, c : c + width].astype(F32) * rate[:, :width] + offset
            half = values * gain[:, c : c + width] + shift[:, c : c + width]
            blocks.append((half * (1.0 + jnp.tanh(half))).astype(BF16))
        hidden = jnp.concatenate(blocks, axis=1) if len(blocks) > 1 else blocks[0]
        at = pl.multiple_of(order_ref[k] * channels, channels)
        part = jnp.dot(hidden, weight_ref[pl.ds(at, channels), :], preferred_element_type=F32)
        total = part if total is None else total + part
    at = 0
    for ref, (low, high) in zip(olds, spans):
        size = high - low
        out_ref[at : at + size, :] = (
            ref[low:high, :].astype(F32) + total[at : at + size, :]
        ).astype(BF16)
        at += size


def emit(order, out_matrix, shards, olds):
    count = len(shards)
    rows = shards[0].shape[0] - TAIL
    channels = shards[0].shape[1]
    width = out_matrix.shape[1]
    spans = [(low, high) for _, low, high in olds]
    return pl.pallas_call(
        functools.partial(emit_body, spans=spans, count=count, rows=rows),
        out_shape=jax.ShapeDtypeStruct((rows, width), BF16),
        in_specs=[smem()] + vmem(1 + count + len(olds)),
        out_specs=vmem(1)[0],
        cost_estimate=pl.CostEstimate(
            flops=2 * rows * width * channels * count,
            bytes_accessed=2 * (rows + width) * channels * count,
            transcendentals=rows * channels * count,
        ),
        name="emit",
    )(order, out_matrix, *shards, *[p for p, _, _ in olds])


def on_device(
    stream,
    norm_gain,
    value_weight,
    gate_weight,
    kernel,
    kernel_bias,
    chan_gain,
    chan_shift,
    out_weight,
):
    layer_count = kernel.shape[0]
    keep = up_to(kernel.shape[1] - 1, 32)
    rows = stream.shape[0]
    order = source_order(lax.axis_size("tp"))
    current = stream
    for layer in range(layer_count):
        gated, last = project(
            order, norm_gain, value_weight[layer], gate_weight[layer],
            fetched(current), layer, keep,
        )
        earlier = passed_along(last)
        packed = convolve(
            kernel, kernel_bias, chan_gain, chan_shift,
            [(earlier, 0, keep), (gated, 0, rows)], layer, keep,
        )
        current = emit(
            order, out_weight[layer], fetched(packed), [(current, 0, rows)]
        )
    return current


def solution(mesh):
    return jax.shard_map(
        on_device,
        mesh=mesh,
        in_specs=(
            P("sp", "tp"),
            P(),
            P(None, "tp", None),
            P(None, "tp", None),
            P(None, None, "tp"),
            P(None, "tp"),
            P(None, "tp"),
            P(None, "tp"),
            P(None, None, "tp"),
        ),
        out_specs=P("sp", "tp"),
        check_vma=False,
    )
```
